128 devices in a mesh: fs: 16 (over z, y), tp: 8 (over x, core).
Axes of the slice: x: 4, y: 4, z: 4, core: 2. Of those that a mesh axis runs over, the one named last changes fastest.
Arguments:
- resid: bfloat16 [16384, 2048], P(('fs', 'tp')), may hold values from -6 to 6
- mix_gain: float32 [2048], replicated, may hold values from 0.1 to 1.9
- w_query: bfloat16 [2048, 1024], P('fs', 'tp'), may hold values from -0.125 to 0.125
- w_key: bfloat16 [2048, 1024], P('fs', 'tp'), may hold values from -0.125 to 0.125
- w_value: bfloat16 [2048, 2048], P('fs', 'tp'), may hold values from -0.125 to 0.125
- w_gate: bfloat16 [2048, 2048], P('fs', 'tp'), may hold values from -0.125 to 0.125
- w_output: bfloat16 [2048, 2048], P('tp', 'fs'), may hold values from -0.125 to 0.125
- decay_rate: float32 [8], P('tp'), may hold values from 0.0008 to 0.034, as said below
- mlp_gain: float32 [2048], replicated, may hold values from 0.1 to 1.9
- w_up: bfloat16 [2048, 8192], P('fs', 'tp'), may hold values from -0.125 to 0.125
- w_down: bfloat16 [8192, 2048], P('tp', 'fs'), may hold values from -0.0625 to 0.0625
Outputs:
- layer_out: bfloat16 [16384, 2048], P(('fs', 'tp'))
The draws below stay inside these ranges and needn't reach their ends.
Inputs may be any that keep to these rules, and one draw needn't show every extreme that they name: `decay_rate`: decay rates per position, one for each head.
All inputs are finite; a program needn't handle non-finite values.
Results may differ from the reference program's by a relative error of at most 0.038.
Values may be sent and summed in bfloat16 or wider, within the bound.
No kernel may reach another device: no remote copies, remote signals or barrier semaphores. Data moves between devices by JAX's collectives and lax.ppermute only.
A program may use at most 64 MiB of HBM per device.

```python
import jax
import jax.numpy as jnp
from jax import lax

D = 2048
HEADS = 8
DK = 128
DV = 256
FF = 8192
BLOCK = 128
LENGTH = 512
TOKENS = 16384
N_TP = 8


def draw_decay_rate(key, part):
    order_key, quick_key, slow_key = jax.random.split(key, 3)
    ranking = jax.random.permutation(order_key, HEADS)
    quick_rate = jnp.exp(jax.random.uniform(quick_key, (HEADS,), jnp.float32, jnp.log(1.0 / 50.0), jnp.log(1.0 / 30.0)))
    slow_rate = jax.random.uniform(slow_key, (HEADS,), jnp.float32, 0.2, 1.0) * (2.3 / LENGTH)
    return jnp.where(ranking < HEADS // 2, quick_rate, slow_rate)


def levels(rng, shape, cuts, low, largest):
    def one(position, shards_of):
        draws = jax.random.uniform(jax.random.fold_in(jax.random.fold_in(rng, 6), position), (shards_of,), jnp.float32, low / len(cuts), largest / len(cuts))
        return jnp.repeat(jnp.exp(draws), shape[position] // shards_of).reshape((-1,) + (1,) * (len(shape) - position - 1))

    level = one(*cuts[0])
    for cut in cuts[1:]:
        level = level * one(*cut)
    return level


def scatter_about(own_key, shape, scale, limit, pieces=(), held_as=jnp.bfloat16):
    drawn = jax.random.normal(own_key, shape, jnp.float32) * scale
    if len(pieces) > 0:
        drawn = levels(own_key, shape, pieces, -0.22, 0.18) * drawn
    return jnp.clip(drawn, min=-limit, max=limit).astype(held_as)


def setup_inputs(seed: int = 0) -> dict:
    key_list = jax.random.split(jax.random.key(seed), 12)
    resid = scatter_about(key_list[0], (TOKENS, D), 1.0, 6.0, ((0, 128),))
    mix_gain = jnp.clip(1.0 + 0.18 * jax.random.normal(key_list[1], (D,), jnp.float32), 0.1, 1.9)
    w_query = scatter_about(key_list[2], (D, HEADS * DK), D ** -0.5, 0.125, ((0, 16), (1, 8)))
    w_key = scatter_about(key_list[3], (D, HEADS * DK), D ** -0.5, 0.125, ((0, 16), (1, 8)))
    w_value = scatter_about(key_list[4], (D, HEADS * DV), D ** -0.5, 0.125, ((0, 16), (1, 8)))
    w_gate = scatter_about(key_list[5], (D, HEADS * DV), D ** -0.5, 0.125, ((0, 16), (1, 8)))
    w_output = scatter_about(key_list[6], (HEADS * DV, D), (HEADS * DV) ** -0.5, 0.125, ((0, 8), (1, 16)))
    decay_rate = draw_decay_rate(jax.random.fold_in(key_list[11], 71), 0)
    mlp_gain = jnp.clip(1.0 + 0.18 * jax.random.normal(key_list[8], (D,), jnp.float32), 0.1, 1.9)
    w_up = scatter_about(key_list[9], (D, FF), D ** -0.5, 0.125, ((0, 16), (1, 8)))
    w_down = scatter_about(key_list[10], (FF, D), FF ** -0.5, 0.0625, ((0, 8), (1, 16)))
    return dict(resid=resid, mix_gain=mix_gain, w_query=w_query, w_key=w_key, w_value=w_value, w_gate=w_gate, w_output=w_output, decay_rate=decay_rate, mlp_gain=mlp_gain, w_up=w_up, w_down=w_down)


epsilon = 1e-06

def rms_scale(source, gains):
    widened = source.astype(jnp.float32)
    scaled = widened * lax.rsqrt(lax.optimization_barrier(jnp.mean(widened * widened, axis=-1, keepdims=True)) + epsilon)
    return (scaled * gains).astype(jnp.bfloat16)

def retention(queries, key_rows, values, rates):
    seq_count, length, head_count, key_width = queries.shape
    value_width = values.shape[-1]
    block_count = length // BLOCK
    queries = queries.reshape(seq_count, block_count, BLOCK, head_count, key_width)
    key_rows = key_rows.reshape(seq_count, block_count, BLOCK, head_count, key_width) * key_width ** (-0.5)
    values = values.reshape(seq_count, block_count, BLOCK, head_count, value_width)
    places = jnp.arange(BLOCK, dtype=jnp.float32)
    offset = places[:, None] - places[None, :]
    causal = offset >= 0
    inner_decay = jnp.where(causal[None], jnp.exp(-rates[:, None, None] * jnp.where(causal, offset, 0.0)[None]), 0.0)
    scores = jnp.einsum('bnihd,bnjhd->bnhij', queries, key_rows) * inner_decay[None, None]
    within = jnp.einsum('bnhij,bnjhe->bnihe', scores, values)
    key_decayed = key_rows * jnp.exp(-rates[None, :] * (BLOCK - 1.0 - places)[:, None])[None, None, :, :, None]
    updates = jnp.einsum('bnjhd,bnjhe->nbhde', key_decayed, values)
    carry_decay = jnp.exp(-rates * BLOCK)[None, :, None, None]

    def advance(memory, update):
        return (carry_decay * memory + update, memory)
    _, before = lax.scan(advance, jnp.zeros((seq_count, head_count, key_width, value_width), jnp.float32), updates)
    query_decayed = queries * jnp.exp(-rates[None, :] * (places + 1.0)[:, None])[None, None, :, :, None]
    carried = jnp.einsum('bnihd,nbhde->bnihe', query_decayed, before)
    mixed = (within + carried).reshape(seq_count, length, head_count, value_width)
    centre = lax.optimization_barrier(jnp.mean(mixed, axis=-1, keepdims=True))
    spread = lax.optimization_barrier(jnp.mean(jnp.square(mixed - centre), axis=-1, keepdims=True))
    return (mixed - centre) * lax.rsqrt(spread + epsilon)

def heads_view(source, width):
    return source.astype(jnp.float32).reshape(-1, LENGTH, source.shape[1] // width, width)

def grouped_sum(left, right):
    group = left.shape[1] // N_TP
    result = jnp.zeros((left.shape[0], right.shape[1]), jnp.float32)
    for member in range(N_TP):
        partial_sum = jnp.dot(left[:, member * group:(member + 1) * group], right[member * group:(member + 1) * group], preferred_element_type=jnp.float32)
        result = result + lax.optimization_barrier(partial_sum.astype(jnp.bfloat16)).astype(jnp.float32)
    return result

def reference(resid, mix_gain, w_query, w_key, w_value, w_gate, w_output, decay_rate, mlp_gain, w_up, w_down):
    tokens = resid.shape[0]
    normed = rms_scale(resid, mix_gain)

    def project(weight):
        return jnp.dot(normed, weight, preferred_element_type=jnp.float32).astype(jnp.bfloat16)
    queries = project(w_query)
    key_rows = project(w_key)
    values = project(w_value)
    gate_rows = project(w_gate)
    grouped = retention(heads_view(queries, DK), heads_view(key_rows, DK), heads_view(values, DV), decay_rate)
    gated = (jax.nn.silu(gate_rows.astype(jnp.float32)) * grouped.reshape(tokens, -1)).astype(jnp.bfloat16)
    mix_sum = grouped_sum(gated, w_output)
    after_mix = (resid.astype(jnp.float32) + mix_sum).astype(jnp.bfloat16)
    normed_mlp = rms_scale(after_mix, mlp_gain)
    lifted = jnp.dot(normed_mlp, w_up, preferred_element_type=jnp.float32)
    hidden = jnp.square(jax.nn.relu(lifted)).astype(jnp.bfloat16)
    mlp_sum = grouped_sum(hidden, w_down)
    return (after_mix.astype(jnp.float32) + mlp_sum).astype(jnp.bfloat16)
```

```python
import jax
import jax.numpy as jnp
from jax import lax
from jax.experimental import pallas as pl
from jax.experimental.pallas import tpu as pltpu
from jax.sharding import PartitionSpec as P


DK = 128
DV = 256
LENGTH = 512
D = 2048
B = 128
NB = 16
EPS = 1e-06
F32 = jnp.float32
BF16 = jnp.bfloat16
VMEM = pl.BlockSpec(memory_space=pltpu.VMEM)
SMEM = pl.BlockSpec(memory_space=pltpu.SMEM)


def from_y(value, step):
    return lax.ppermute(
        value, "fs", [(z * 4 + (y + step) % 4, z * 4 + y) for z in range(4) for y in range(4)]
    )


def from_z(value, step):
    return lax.ppermute(
        value, "fs", [((z + step) % 4 * 4 + y, z * 4 + y) for z in range(4) for y in range(4)]
    )


def from_x(value, step):
    return lax.ppermute(
        value, "tp", [((x + step) % 4 * 2 + c, x * 2 + c) for x in range(4) for c in range(2)]
    )


def from_partner(value):
    return lax.ppermute(value, "tp", [(x * 2 + 1 - c, x * 2 + c) for x in range(4) for c in range(2)])


def kernel_call(body, outs, specs, name, scratch=(), limit=None):
    return pl.pallas_call(
        body,
        out_shape=outs,
        in_specs=specs,
        out_specs=jax.tree.map(lambda _: VMEM, outs),
        scratch_shapes=list(scratch),
        compiler_params=pltpu.CompilerParams(vmem_limit_bytes=limit),
        name=name,
    )


def lanes(block):
    return pl.ds(pl.multiple_of(block * B, B), B)


def norm_in(src, resid, gain):
    def body(src_ref, resid_ref, gain_ref, normed_ref, turned_ref):
        total = jnp.zeros((B, B), F32)
        for b in range(NB):
            part = resid_ref[:, b * B : (b + 1) * B].astype(F32)
            total = total + part * part
        scale = lax.rsqrt(jnp.sum(total, axis=1, keepdims=True) / D + EPS)
        for b in range(NB):
            s = src_ref[b]
            part = resid_ref[:, lanes(s)]
            turned_ref[:, b * B : (b + 1) * B] = part
            normed_ref[:, b * B : (b + 1) * B] = (
                part.astype(F32) * scale * gain_ref[pl.ds(s, 1), :]
            ).astype(BF16)

    shape = jax.ShapeDtypeStruct(resid.shape, BF16)
    return kernel_call(body, (shape, shape), [SMEM, VMEM, VMEM], "norm_in")(src, resid, gain)


def norm_mid(src, turned, parts, gain):
    def body(src_ref, turned_ref, p0, p1, p2, p3, gain_ref, normed_ref, after_ref):
        total = jnp.zeros((B, B), F32)
        for b in range(NB):
            cols = slice(b * B, (b + 1) * B)
            mix = (p0[:, cols].astype(F32) + p1[:, cols].astype(F32)) + (
                p2[:, cols].astype(F32) + p3[:, cols].astype(F32)
            )
            after = (turned_ref[:, cols].astype(F32) + mix).astype(BF16)
            after_ref[:, cols] = after
            wide = after.astype(F32)
            total = total + wide * wide
        scale = lax.rsqrt(jnp.sum(total, axis=1, keepdims=True) / D + EPS)
        for b in range(NB):
            cols = slice(b * B, (b + 1) * B)
            normed_ref[:, cols] = (
                after_ref[:, cols].astype(F32) * scale * gain_ref[pl.ds(src_ref[b], 1), :]
            ).astype(BF16)

    shape = jax.ShapeDtypeStruct(turned.shape, BF16)
    return kernel_call(body, (shape, shape), [SMEM] + [VMEM] * 6, "norm_mid")(
        src, turned, *parts, gain
    )


def add_out(src, after, parts):
    def body(src_ref, after_ref, p0, p1, p2, p3, out_ref):
        for b in range(NB):
            cols = slice(b * B, (b + 1) * B)
            mlp = (p0[:, cols].astype(F32) + p1[:, cols].astype(F32)) + (
                p2[:, cols].astype(F32) + p3[:, cols].astype(F32)
            )
            out_ref[:, lanes(src_ref[b])] = (after_ref[:, cols].astype(F32) + mlp).astype(BF16)

    return kernel_call(
        body, jax.ShapeDtypeStruct(after.shape, BF16), [SMEM] + [VMEM] * 5, "add_out"
    )(src, after, *parts)


def mixer(place, rate, own, other, qv, kg):
    def body(place_ref, rate_ref, *refs):
        own_refs, other_refs, qv_refs, kg_refs = refs[:4], refs[4:8], refs[8:12], refs[12:16]
        mine_ref, send_ref, x_ref, qk_ref, vg_ref, gated_ref = refs[16:]
        for dx in range(4):
            x_ref[pl.ds(pl.multiple_of(place_ref[dx] * B, B), B), :] = own_refs[dx][...]
            x_ref[pl.ds(pl.multiple_of(place_ref[4 + dx] * B, B), B), :] = other_refs[dx][...]

        def project(step, _):
            rows = pl.ds(pl.multiple_of(step * 256, 256), 256)
            acc = jnp.zeros((256, 384), F32)
            for dz in range(4):
                acc = acc + jnp.dot(
                    x_ref[rows, dz * 512 : (dz + 1) * 512],
                    qv_refs[dz][...],
                    preferred_element_type=F32,
                )
            qk_ref[rows, :128] = acc[:, :128].astype(BF16)
            vg_ref[rows, :256] = acc[:, 128:].astype(BF16)
            acc = jnp.zeros((256, 384), F32)
            for dy in range(4):
                left = jnp.concatenate(
                    [x_ref[rows, (dz * 4 + dy) * B : (dz * 4 + dy + 1) * B] for dz in range(4)],
                    axis=1,
                )
                acc = acc + jnp.dot(left, kg_refs[dy][...], preferred_element_type=F32)
            qk_ref[rows, 128:] = acc[:, :128].astype(BF16)
            vg_ref[rows, 256:] = acc[:, 128:].astype(BF16)
            return 0

        lax.fori_loop(0, 4, project, 0)
        gap = (
            lax.broadcasted_iota(jnp.int32, (B, LENGTH), 0)
            - lax.broadcasted_iota(jnp.int32, (B, LENGTH), 1)
            + (LENGTH - B)
        )
        decay = jnp.where(
            gap >= 0, jnp.exp(-rate_ref[0] * jnp.maximum(gap, 0).astype(F32)), 0.0
        )
        for seq in range(2):
            base = seq * LENGTH
            for i in range(4):
                rows = slice(base + i * B, base + (i + 1) * B)
                seen = slice(base, base + (i + 1) * B)
                scores = lax.dot_general(
                    qk_ref[rows, :128],
                    qk_ref[seen, 128:],
                    (((1,), (1,)), ((), ())),
                    preferred_element_type=F32,
                )
                scores = scores * (DK**-0.5) * decay[:, (3 - i) * B :]
                kept = jnp.dot(scores.astype(BF16), vg_ref[seen, :256], preferred_element_type=F32)
                centred = kept - jnp.mean(kept, axis=1, keepdims=True)
                spread = jnp.mean(centred * centred, axis=1, keepdims=True)
                gate = vg_ref[rows, 256:].astype(F32)
                gated_ref[seq * 4 + i] = (
                    gate / (1.0 + jnp.exp(-gate)) * (centred * lax.rsqrt(spread + EPS))
                ).astype(BF16)
        for dx in range(4):
            mine_ref[dx] = gated_ref[place_ref[dx]]
            send_ref[dx] = gated_ref[place_ref[4 + dx]]

    shape = jax.ShapeDtypeStruct((4, B, DV), BF16)
    return kernel_call(
        body,
        (shape, shape),
        [SMEM, SMEM] + [VMEM] * 16,
        "mixer",
        scratch=(
            pltpu.VMEM((1024, D), BF16),
            pltpu.VMEM((1024, 256), BF16),
            pltpu.VMEM((1024, 512), BF16),
            pltpu.VMEM((8, B, DV), BF16),
        ),
        limit=32 << 20,
    )(place, rate, *own, *other, *qv, *kg)


def output_product(src, mine, theirs, w_mine, w_theirs):
    def body(src_ref, mine_ref, theirs_ref, wm_ref, wt_ref, *outs):
        left_m = mine_ref[...].reshape(4 * B, DV)
        left_t = theirs_ref[...].reshape(4 * B, DV)
        for b in range(0, NB, 2):
            s, t = src_ref[b], src_ref[b + 1]
            acc = jnp.dot(
                left_m, jnp.concatenate([wm_ref[s], wm_ref[t]], axis=1), preferred_element_type=F32
            ) + jnp.dot(
                left_t, jnp.concatenate([wt_ref[s], wt_ref[t]], axis=1), preferred_element_type=F32
            )
            for dx in range(4):
                outs[dx][:, b * B : (b + 2) * B] = acc[dx * B : (dx + 1) * B].astype(BF16)

    shape = jax.ShapeDtypeStruct((B, D), BF16)
    return kernel_call(body, (shape,) * 4, [SMEM] + [VMEM] * 4, "output_product", limit=24 << 20)(
        src, mine, theirs, w_mine, w_theirs
    )


def mlp(blocks, up, up_other, down, down_other):
    count = len(blocks)
    rows = count * B
    flat_up = [p for group in (up, up_other) for pieces in group for p in pieces]
    flat_down = [p for group in (down, down_other) for pieces in group for p in pieces]
    up_sizes = [[p.shape[0] for p in pieces] for pieces in up]
    down_sizes = [[p.shape[0] for p in pieces] for pieces in down]

    def body(*refs):
        refs = list(refs)
        x_refs = [refs.pop(0) for _ in range(count)]
        ups = [[[refs.pop(0) for _ in sizes] for sizes in up_sizes] for _ in range(2)]
        downs = [[[refs.pop(0) for _ in sizes] for sizes in down_sizes] for _ in range(2)]
        outs = [refs.pop(0) for _ in range(count)]
        hid_ref = refs.pop(0)

        def left(lo, size):
            if count == 1:
                return x_refs[0][:, lo : lo + size]
            return jnp.concatenate([r[:, lo : lo + size] for r in x_refs], axis=0)

        for core in range(2):

            def lift(step, _):
                cols = pl.ds(pl.multiple_of(step * 256, 256), 256)
                acc = jnp.zeros((rows, 256), F32)
                at = 0
                for dz in range(4):
                    for ref, size in zip(ups[core][dz], up_sizes[dz]):
                        acc = acc + jnp.dot(left(at, size), ref[:, cols], preferred_element_type=F32)
                        at += size
                acc = jnp.maximum(acc, 0.0)
                hid_ref[:, pl.ds(pl.multiple_of(step * 256 + core * 1024, 256), 256)] = (
                    acc * acc
                ).astype(BF16)
                return 0

            lax.fori_loop(0, 4, lift, 0)
        for dy in range(4):
            for half in range(2):
                acc = jnp.zeros((rows, 256), F32)
                for core in range(2):
                    planes = [
                        (ref, k)
                        for ref, size in zip(downs[core][dy], down_sizes[dy])
                        for k in range(size)
                    ]
                    right = jnp.concatenate(
                        [planes[2 * half + k][0][planes[2 * half + k][1]] for k in range(2)], axis=1
                    )
                    acc = acc + jnp.dot(
                        hid_ref[:, core * 1024 : (core + 1) * 1024],
                        right,
                        preferred_element_type=F32,
                    )
                for k in range(2):
                    b = (2 * half + k) * 4 + dy
                    for n in range(count):
                        outs[n][:, b * B : (b + 1) * B] = acc[
                            n * B : (n + 1) * B, k * B : (k + 1) * B
                        ].astype(BF16)

    shape = jax.ShapeDtypeStruct((B, D), BF16)
    return kernel_call(
        body,
        (shape,) * count,
        [VMEM] * (count + len(flat_up) + len(flat_down)),
        "mlp",
        scratch=(pltpu.VMEM((rows, D), BF16),),
        limit=40 << 20,
    )(*blocks, *flat_up, *flat_down)


def gather_pair(value, first, second, join, halve):
    near, far, back = first(value, 1), first(value, 2), first(value, -1)
    stack = join([value, near, far, back])
    up = second(stack, 1)
    down = second(stack, -1)
    if halve is None:
        return [[stack], [up], [second(stack, 2)], [down]]
    low = second(halve(up, 0), 1)
    high = second(halve(down, 1), -1)
    return [[stack], [up], [low, high], [down]]


def on_device(
    resid, mix_gain, w_query, w_key, w_value, w_gate, w_output, decay_rate, mlp_gain, w_up, w_down
):
    f = lax.axis_index("fs")
    t = lax.axis_index("tp")
    z, y, x, c = f // 4, f % 4, t // 2, t % 2
    b = jnp.arange(NB, dtype=jnp.int32)
    src = (z + b // 4) % 4 * 4 + (y + b % 4) % 4
    d = jnp.arange(8, dtype=jnp.int32)
    place = (x + d) % 4 * 2 + jnp.where(d < 4, c, 1 - c)

    def rows_join(pieces):
        return jnp.concatenate(pieces, axis=0)

    def rows_half(value, k):
        half = value.shape[0] // 2
        return value[k * half : (k + 1) * half]

    normed, turned = norm_in(src, resid, mix_gain.reshape(NB, B))
    qv = gather_pair(jnp.concatenate([w_query, w_value], axis=1), from_y, from_z, rows_join, None)
    kg = gather_pair(jnp.concatenate([w_key, w_gate], axis=1), from_z, from_y, rows_join, None)
    own = [normed, from_x(normed, 1), from_x(normed, 2), from_x(normed, -1)]
    other = [from_partner(v) for v in own]

    out_mine = lax.all_to_all(
        jnp.broadcast_to(w_output[None], (NB, *w_output.shape)), "fs", 0, 0, tiled=True
    )
    out_theirs = from_partner(out_mine)

    tied_up, tied_down, _, _ = lax.optimization_barrier((w_up, w_down, qv[0][0], kg[0][0]))
    up = gather_pair(tied_up, from_y, from_z, rows_join, rows_half)
    down = gather_pair(tied_down[None], from_z, from_y, rows_join, rows_half)
    up_other = [[from_partner(p) for p in pieces] for pieces in up]
    down_other = [[from_partner(p) for p in pieces] for pieces in down]

    mine, send = mixer(place, decay_rate, own, other, [p[0] for p in qv], [p[0] for p in kg])
    theirs = from_partner(send)
    p0, p1, p2, p3 = output_product(src, mine, theirs, out_mine, out_theirs)
    normed_mlp, after = norm_mid(
        src,
        turned,
        (p0, from_x(p1, -1), from_x(p2, 2), from_x(p3, 1)),
        mlp_gain.reshape(NB, B),
    )
    n1, n2, n3 = from_x(normed_mlp, 1), from_x(normed_mlp, 2), from_x(normed_mlp, -1)
    o1, o3 = mlp([n1, n3], up, up_other, down, down_other)
    (o2,) = mlp([n2], up, up_other, down, down_other)
    (o0,) = mlp([normed_mlp], up, up_other, down, down_other)
    return add_out(src, after, (o0, from_x(o1, -1), from_x(o2, 2), from_x(o3, 1)))


def solution(mesh):
    placed = (
        P(("fs", "tp"), None),
        P(),
        P("fs", "tp"),
        P("fs", "tp"),
        P("fs", "tp"),
        P("fs", "tp"),
        P("tp", "fs"),
        P("tp"),
        P(),
        P("fs", "tp"),
        P("tp", "fs"),
    )
    return jax.shard_map(
        on_device, mesh=mesh, in_specs=placed, out_specs=P(("fs", "tp"), None), check_vma=False
    )
```
